32 devices in a mesh: sp: 16 (over z, y, x), tp: 2 (over core).
Axes of the slice: x: 2, y: 2, z: 4, core: 2. Of those that a mesh axis runs over, the one named last changes fastest.
Arguments:
- stream: bfloat16 [2048, 2048], P('sp'), may hold values from -6 to 6
- query_narrow: bfloat16 [2048, 512], P('sp', 'tp'), may hold values from -7 to 7
- query_broad: bfloat16 [2048, 1024], P('sp', 'tp'), may hold values from -7 to 7
- key_narrow: bfloat16 [2048, 512], P('sp', 'tp'), may hold values from -7 to 7
- key_broad: bfloat16 [2048, 1024], P('sp', 'tp'), may hold values from -7 to 7
- value_narrow: bfloat16 [2048, 512], P('sp', 'tp'), may hold values from -6 to 6
- value_broad: bfloat16 [2048, 1024], P('sp', 'tp'), may hold values from -6 to 6
- key_offsets: float32 [2048, 16], P('sp', 'tp'), may hold values from -20 to 0
- out_narrow: bfloat16 [512, 2048], P('tp'), may hold values from -0.4375 to 0.4375
- out_broad: bfloat16 [1024, 2048], P('tp'), may hold values from -0.4375 to 0.4375
- norm_gain: float32 [2048], replicated, may hold values from 0.1 to 1.9
- gate_weight: bfloat16 [2048, 3072], P('sp', 'tp'), may hold values from -0.125 to 0.125
- up_weight: bfloat16 [2048, 3072], P('sp', 'tp'), may hold values from -0.125 to 0.125
- down_weight: bfloat16 [3072, 2048], P('tp', 'sp'), may hold values from -0.21875 to 0.21875
Outputs:
- result: bfloat16 [2048, 2048], P(('sp', 'tp'))
The draws below stay inside these ranges and needn't reach their ends.
All inputs are finite; a program needn't handle non-finite values.
Results may differ from the reference program's by a relative error of at most 0.028.
Values may be sent and summed in bfloat16 or wider, within the bound.
No kernel may reach another device: no remote copies, remote signals or barrier semaphores. Data moves between devices by JAX's collectives and lax.ppermute only.
A program may use at most 64 MiB of HBM per device.

```python
import jax
import jax.numpy as jnp
from jax import lax

D = 2048
FF = 3072
NARROW_HEADS = 8
NARROW_SIZE = 64
BROAD_HEADS = 8
BROAD_SIZE = 128
TOK_DEV = 128
SEQUENCE_TOKENS = 2048
N_TP = 2


def draw_key_offsets(key, part):
    parallel_flows = jax.random.split(jax.random.fold_in(key, 17), 6)
    column_indices = 2 * NARROW_HEADS
    fast_share = 0.5
    spread = 0.7
    fast = jax.random.uniform(parallel_flows[0], (column_indices,), jnp.float32) < fast_share
    slow_base = -2.0 - jnp.log(jnp.float32(SEQUENCE_TOKENS)) + jax.random.uniform(parallel_flows[1], (column_indices,), jnp.float32, -0.5, 0.5)
    base = jnp.where(fast, -3.5, slow_base)
    shifts = jax.random.uniform(parallel_flows[2], (SEQUENCE_TOKENS // TOK_DEV, 1, column_indices), jnp.float32, -spread, spread)
    moved_forward = (base[None, None, :] + shifts + jnp.zeros((SEQUENCE_TOKENS // TOK_DEV, TOK_DEV, column_indices), jnp.float32)).reshape(SEQUENCE_TOKENS, column_indices)
    coarse_estimate = jax.random.uniform(parallel_flows[3], (SEQUENCE_TOKENS, column_indices), jnp.float32, -0.5, 0.5)
    arrival_group = jax.random.uniform(parallel_flows[4], (SEQUENCE_TOKENS, column_indices), jnp.float32) < 4.0 / SEQUENCE_TOKENS
    arrival_value = jax.random.uniform(parallel_flows[5], (SEQUENCE_TOKENS, column_indices), jnp.float32, -2.5, -1.0)
    return jnp.where(arrival_group, arrival_value, moved_forward + coarse_estimate).astype(jnp.float32)


def steps_of(own_key, dims, shards, low, high):
    factor_of, own = 1.0, jax.random.fold_in(own_key, 6)
    for position, blocks in shards:
        steps = jnp.exp(jax.random.uniform(jax.random.fold_in(own, position), (blocks,), jnp.float32, low / len(shards), high / len(shards)))
        factor_of = factor_of * jnp.repeat(steps, dims[position] // blocks).reshape([-1 if axis == position else 1 for axis in range(len(dims))])
    return factor_of


def noise(key, extent, width, limit, cuts=(), kind=jnp.bfloat16):
    array = jax.random.normal(key, extent, jnp.float32) * width
    if len(cuts) > 0:
        array = steps_of(key, extent, cuts, -0.22, 0.18) * array
    return jnp.clip(array, min=-limit, max=limit).astype(kind)


def setup_inputs(seed: int = 0) -> dict:
    seeds = jax.random.split(jax.random.key(seed), 15)
    return {
        "stream": noise(seeds[0], (SEQUENCE_TOKENS, D), 1.0, 6.0, ((0, 16),)),
        "query_narrow": noise(seeds[1], (SEQUENCE_TOKENS, NARROW_HEADS * NARROW_SIZE), 1.2, 7.0, ((0, 16), (1, 2))),
        "query_broad": noise(seeds[2], (SEQUENCE_TOKENS, BROAD_HEADS * BROAD_SIZE), 1.2, 7.0, ((0, 16), (1, 2))),
        "key_narrow": noise(seeds[3], (SEQUENCE_TOKENS, NARROW_HEADS * NARROW_SIZE), 1.2, 7.0, ((0, 16), (1, 2))),
        "key_broad": noise(seeds[4], (SEQUENCE_TOKENS, BROAD_HEADS * BROAD_SIZE), 1.2, 7.0, ((0, 16), (1, 2))),
        "value_narrow": noise(seeds[5], (SEQUENCE_TOKENS, NARROW_HEADS * NARROW_SIZE), 1.0, 6.0, ((0, 16), (1, 2))),
        "value_broad": noise(seeds[6], (SEQUENCE_TOKENS, BROAD_HEADS * BROAD_SIZE), 1.0, 6.0, ((0, 16), (1, 2))),
        "key_offsets": draw_key_offsets(jax.random.fold_in(seeds[14], 71), 0),
        "out_narrow": noise(seeds[8], (NARROW_HEADS * NARROW_SIZE, D), ((NARROW_HEADS * NARROW_SIZE + BROAD_HEADS * BROAD_SIZE) // 9) ** -0.5, 0.4375, ((0, 2),)),
        "out_broad": noise(seeds[9], (BROAD_HEADS * BROAD_SIZE, D), ((NARROW_HEADS * NARROW_SIZE + BROAD_HEADS * BROAD_SIZE) // 9) ** -0.5, 0.4375, ((0, 2),)),
        "norm_gain": jnp.clip(1.0 + 0.18 * jax.random.normal(seeds[10], (D,), jnp.float32), 0.1, 1.9),
        "gate_weight": noise(seeds[11], (D, FF), D ** -0.5, 0.125, ((0, 16), (1, 2))),
        "up_weight": noise(seeds[12], (D, FF), D ** -0.5, 0.125, ((0, 16), (1, 2))),
        "down_weight": noise(seeds[13], (FF, D), (FF // 4) ** -0.5, 0.21875, ((0, 2), (1, 16))),
    }


def stick_heads(query, keys, values, offsets, heads, size):
    total = query.shape[0]
    qblock = 512 if total % 512 == 0 else total
    scale = size ** (-0.5)
    pieces = []
    for head in range(heads):
        query_head = query[:, head * size:(head + 1) * size]
        key_head = keys[:, head * size:(head + 1) * size]
        value_head = values[:, head * size:(head + 1) * size]
        offset_head = offsets[:, head]

        def one_block(index):
            first = (index * qblock).astype(jnp.int32)
            rows_q = lax.dynamic_slice_in_dim(query_head, first, qblock, 0)
            logits = jnp.dot(rows_q, jnp.transpose(key_head), preferred_element_type=jnp.float32) * scale + offset_head[None, :]
            tpos = first + jnp.arange(qblock, dtype=jnp.int32)
            spos = jnp.arange(total, dtype=jnp.int32)
            causal = spos[None, :] < tpos[:, None]
            lognot = jnp.where(causal, jax.nn.log_sigmoid(-logits), 0.0)
            later = lax.cumsum(lognot, axis=1, reverse=True) - lognot
            weights = jnp.where(causal, jnp.exp(jax.nn.log_sigmoid(logits) + later), 0.0).astype(jnp.bfloat16)
            return jnp.dot(weights, value_head, preferred_element_type=jnp.float32)
        blocks = lax.map(one_block, jnp.arange(total // qblock, dtype=jnp.int32))
        pieces.append(blocks.reshape(total, size).astype(jnp.bfloat16))
    return jnp.concatenate(pieces, axis=1)

def rounded(value):
    return lax.optimization_barrier(value.astype(jnp.bfloat16)).astype(jnp.float32)

def reference(stream, query_narrow, query_broad, key_narrow, key_broad, value_narrow, value_broad, key_offsets, out_narrow, out_broad, norm_gain, gate_weight, up_weight, down_weight):
    attended_narrow = stick_heads(query_narrow, key_narrow, value_narrow, key_offsets[:, 0::2], NARROW_HEADS, NARROW_SIZE)
    attended_broad = stick_heads(query_broad, key_broad, value_broad, key_offsets[:, 1::2], BROAD_HEADS, BROAD_SIZE)
    width_narrow = NARROW_HEADS // N_TP * NARROW_SIZE
    width_broad = BROAD_HEADS // N_TP * BROAD_SIZE
    total = jnp.zeros((stream.shape[0], D), jnp.float32)
    for index in range(N_TP):
        part = jnp.dot(attended_narrow[:, index * width_narrow:(index + 1) * width_narrow], out_narrow[index * width_narrow:(index + 1) * width_narrow], preferred_element_type=jnp.float32)
        part = part + jnp.dot(attended_broad[:, index * width_broad:(index + 1) * width_broad], out_broad[index * width_broad:(index + 1) * width_broad], preferred_element_type=jnp.float32)
        total = total + rounded(part)
    mid = (stream.astype(jnp.float32) + total).astype(jnp.bfloat16)
    middle = mid.astype(jnp.float32)
    normed = (middle * lax.rsqrt(lax.optimization_barrier(jnp.mean(middle * middle, axis=1, keepdims=True)) + 1e-06) * norm_gain).astype(jnp.bfloat16)
    gate = jnp.dot(normed, gate_weight, preferred_element_type=jnp.float32)
    up = jnp.dot(normed, up_weight, preferred_element_type=jnp.float32)
    hidden = (jax.nn.silu(gate) * up).astype(jnp.bfloat16)
    hidden_width = FF // N_TP
    mixed = jnp.zeros((stream.shape[0], D), jnp.float32)
    for index in range(N_TP):
        part = jnp.dot(hidden[:, index * hidden_width:(index + 1) * hidden_width], down_weight[index * hidden_width:(index + 1) * hidden_width], preferred_element_type=jnp.float32)
        mixed = mixed + rounded(part)
    return (middle + mixed).astype(jnp.bfloat16)
```

```python
import functools
import math

import jax
import jax.numpy as jnp
from jax import lax
from jax.experimental import pallas as pl
from jax.experimental.pallas import tpu as pltpu
from jax.sharding import PartitionSpec as P

NARROW_SIZE = 64
BROAD_SIZE = 128
LANES = 128
EXTRA = 8
KV_LANES = 2 * BROAD_SIZE + 2 * NARROW_SIZE
ALL_LANES = KV_LANES + BROAD_SIZE + 2 * NARROW_SIZE
norm_eps = 1e-06
NEG = -1e30
BF = jnp.bfloat16
F32 = jnp.float32
ANY = pl.BlockSpec(memory_space=pl.ANY)
VMEM = pl.BlockSpec(memory_space=pltpu.VMEM)
SMEM = pl.BlockSpec(memory_space=pltpu.SMEM)

TEAM_BITS = (0, 2)
PEER_BITS = (1, 3)


class Plan:
    def __init__(self, sp, tp, heads, hidden):
        self.sp, self.tp = sp, tp
        self.split = sp == 16 and heads % 4 == 0 and hidden % (4 * LANES) == 0
        self.team_bits = TEAM_BITS if self.split else ()
        self.peer_bits = PEER_BITS if self.split else ()
        self.team = 4 if self.split else 1
        self.peers = sp // self.team

    def place(self, value, bits):
        out = 0
        for j, bit in enumerate(bits):
            out = out + (((value >> j) & 1) << bit)
        return out

    def index(self, t, w):
        if not self.split:
            return w
        return self.place(t, self.team_bits) + self.place(w, self.peer_bits)

    def member(self, i):
        if not self.split:
            return i * 0
        return sum(((i >> bit) & 1) << j for j, bit in enumerate(self.team_bits))

    def peer(self, i):
        if not self.split:
            return i
        return sum(((i >> bit) & 1) << j for j, bit in enumerate(self.peer_bits))

    def swap(self, array, offset):
        return lax.ppermute(array, "sp", [(i, i ^ offset) for i in range(self.sp)])

    def team_swap(self, array, r):
        return self.swap(array, self.place(r, self.team_bits))

    def peer_swap(self, array, r):
        return self.swap(array, self.place(r, self.peer_bits))


def pick(array, index):
    return lax.dynamic_index_in_dim(array, index, 0, keepdims=False)


def cost(flops, moved, transcendentals=0):
    return pl.CostEstimate(
        flops=int(flops), bytes_accessed=int(moved), transcendentals=int(transcendentals)
    )


def attention_kernel(plan, me_ref, own_ref, *refs):
    team, rows = plan.team, own_ref.shape[2] - EXTRA
    local_heads = own_ref.shape[1]
    part_count = plan.peers - 1 if plan.split else 1
    parts = refs[:part_count]
    out_ref, kv_s, q_s, acc_s, carry_s, kv_sems, q_sems = refs[part_count:]
    me = me_ref[0]
    t = plan.member(me)
    w = plan.peer(me)
    copies = []
    number = 0
    for h in range(local_heads):
        for r in range(team):
            copies.append(
                pltpu.make_async_copy(
                    own_ref.at[r, h, pl.ds(0, rows), pl.ds(KV_LANES, ALL_LANES - KV_LANES)],
                    q_s.at[h, jnp.bitwise_xor(t, r)],
                    q_sems.at[h * team + r],
                )
            )
        if plan.split:
            for rw in range(plan.peers):
                for r in range(team):
                    source = own_ref if rw == 0 else parts[rw - 1]
                    position = jnp.bitwise_xor(me, plan.index(r, rw))
                    copies.append(
                        pltpu.make_async_copy(
                            source.at[r, h, :, pl.ds(0, KV_LANES)],
                            kv_s.at[h, position],
                            kv_sems.at[number],
                        )
                    )
                    number += 1
        else:
            copies.append(
                pltpu.make_async_copy(parts[0].at[:, h], kv_s.at[h], kv_sems.at[number])
            )
            number += 1
    for copy in copies:
        copy.start()
    acc_s[...] = jnp.zeros_like(acc_s)
    carry_s[...] = jnp.zeros_like(carry_s)
    for copy in copies:
        copy.wait()

    pair = 2 if plan.sp % 2 == 0 else 1
    span = pair * rows
    tri = (
        lax.broadcasted_iota(jnp.int32, (span, span), 0)
        > lax.broadcasted_iota(jnp.int32, (span, span), 1)
    ).astype(F32).astype(BF)
    scales = (BROAD_SIZE ** (-0.5), NARROW_SIZE ** (-0.5))
    group = 2 if team % 2 == 0 else 1
    for first in reversed(range(0, team, group)):
        count = group * rows
        places = [plan.index(k, w) for k in range(first, first + group)]
        query_positions = jnp.concatenate(
            [p * rows + lax.broadcasted_iota(jnp.int32, (rows, span), 0) for p in places], axis=0
        )
        gap = lax.broadcasted_iota(jnp.int32, (count, span), 1) - query_positions
        steps = places[-1] // pair + 1

        def body(step, _, first=first, count=count, gap=gap, steps=steps):
            chunk = steps - 1 - step
            causal = gap < -chunk * span
            for h in range(local_heads):
                tails = [
                    kv_s[h, chunk * pair + b, pl.ds(rows, EXTRA), :].astype(F32)
                    for b in range(pair)
                ]
                tails = [a[:, :rows] + a[:, rows : 2 * rows] + a[:, 2 * rows : 3 * rows] for a in tails]
                offsets = jnp.concatenate(tails, axis=1)
                lanes = kv_s[h, pl.ds(chunk * pair, pair), pl.ds(0, rows), :]
                for g in range(2):
                    keys = lanes[:, :, 2 * LANES * g : 2 * LANES * g + LANES].reshape(span, LANES)
                    values = keys if g else lanes[:, :, LANES : 2 * LANES].reshape(span, LANES)
                    queries = q_s[h, first : first + group, :, g * LANES : (g + 1) * LANES]
                    queries = queries.reshape(count, LANES)
                    logits = lax.dot_general(
                        queries, keys, (((1,), (1,)), ((), ())), preferred_element_type=F32
                    )
                    logits = logits * scales[g] + offsets[g : g + 1]
                    logits = jnp.where(causal, logits, NEG)
                    lognot = jnp.minimum(-logits, 0.0) - jnp.log(1.0 + jnp.exp(-jnp.abs(logits)))
                    later = jnp.dot(lognot.astype(BF), tri, preferred_element_type=F32)
                    here = pl.ds(first * rows, count)
                    carry = carry_s[h, g, here, :]
                    wide = jnp.concatenate([carry] * (span // LANES), axis=1)
                    weights = jnp.exp(logits + lognot + (later + wide)).astype(BF)
                    acc_s[h, g, here, :] += jnp.dot(weights, values, preferred_element_type=F32)
                    carry_s[h, g, here, :] = carry + (later[:, :1] + lognot[:, :1])
            return 0

        lax.fori_loop(0, steps, body, 0)
    for h in range(local_heads):
        for g in range(2):
            out_ref[h, :, g * LANES : (g + 1) * LANES] = acc_s[h, g].astype(BF)


def attention(plan, me, own, parts):
    team, local_heads, tall, _ = own.shape
    rows = tall - EXTRA
    total = team * rows
    pieces = plan.sp if plan.split else 1
    work = local_heads * 2 * total * plan.sp * rows
    return pl.pallas_call(
        functools.partial(attention_kernel, plan),
        out_shape=jax.ShapeDtypeStruct((local_heads, total, 2 * LANES), BF),
        in_specs=[SMEM, ANY] + [ANY] * len(parts),
        out_specs=VMEM,
        scratch_shapes=[
            pltpu.VMEM((local_heads, plan.sp, tall, KV_LANES), BF),
            pltpu.VMEM((local_heads, team, rows, 2 * LANES), BF),
            pltpu.VMEM((local_heads, 2, total, LANES), F32),
            pltpu.VMEM((local_heads, 2, total, LANES), F32),
            pltpu.SemaphoreType.DMA((local_heads * pieces,)),
            pltpu.SemaphoreType.DMA((local_heads * team,)),
        ],
        cost_estimate=cost(work * 4 * LANES, 8 * own.size, 3 * work),
        name="attention",
    )(me, own, *parts)


def project_kernel(plan, me_ref, broad_ref, narrow_ref, *refs):
    team = plan.team
    attended = refs[:team]
    out_ref, a_s, w_s = refs[team:]
    local_heads, total, _ = attended[0].shape
    t = plan.member(me_ref[0])
    depth = out_ref.shape[1]
    for r in range(team):
        for h in range(local_heads):
            at = (r * local_heads + h) * 2 * LANES
            head = jnp.bitwise_xor(t, r) * local_heads + h
            a_s[:, pl.ds(at, 2 * LANES)] = attended[r][h]
            w_s[pl.ds(at, LANES), :] = broad_ref[
                pl.ds(pl.multiple_of(head * BROAD_SIZE, BROAD_SIZE), BROAD_SIZE), :
            ]
            w_s[pl.ds(at + LANES, NARROW_SIZE), :] = jnp.zeros((NARROW_SIZE, depth), BF)
            w_s[pl.ds(at + LANES + NARROW_SIZE, NARROW_SIZE), :] = narrow_ref[
                pl.ds(pl.multiple_of(head * NARROW_SIZE, NARROW_SIZE), NARROW_SIZE), :
            ]
    width = min(512, depth)
    for n in range(0, depth, width):
        out_ref[:, pl.ds(n, width)] = jnp.dot(
            a_s[...], w_s[:, pl.ds(n, width)], preferred_element_type=F32
        ).astype(BF)


def project(plan, me, attended, out_broad, out_narrow):
    local_heads, total, _ = attended[0].shape
    depth = out_broad.shape[1]
    inner = plan.team * local_heads * 2 * LANES
    return pl.pallas_call(
        functools.partial(project_kernel, plan),
        out_shape=jax.ShapeDtypeStruct((total, depth), BF),
        in_specs=[SMEM] + [VMEM] * (2 + len(attended)),
        out_specs=VMEM,
        scratch_shapes=[pltpu.VMEM((total, inner), BF), pltpu.VMEM((inner, depth), BF)],
        cost_estimate=cost(2 * total * inner * depth, 2 * total * depth),
        name="project",
    )(me, out_broad, out_narrow, *attended)


def mixer_kernel(plan, gate_parts, down_parts, me_ref, gain_ref, mine_ref, other_ref, *refs):
    team, tp = plan.team, plan.tp
    streams = refs[:team]
    refs = refs[team:]
    gates, refs = refs[:gate_parts], refs[gate_parts:]
    downs, refs = refs[:down_parts], refs[down_parts:]
    mid_ref, mixed_ref, gu_s, down_s, normed_s, mid_s, gu_sems, down_sems = refs
    me, core = me_ref[0], me_ref[1]
    t = plan.member(me)
    rows, depth = streams[0].shape
    band = gu_s.shape[0] // plan.sp
    units = down_s.shape[0]
    column = depth // plan.sp
    gate_copies, down_copies = [], []
    if plan.split:
        for rw in range(plan.peers):
            for r in range(team):
                place = jnp.bitwise_xor(me, plan.index(r, rw))
                number = rw * team + r
                gate_copies.append(
                    pltpu.make_async_copy(
                        gates[rw].at[r],
                        gu_s.at[pl.ds(pl.multiple_of(place * band, band), band), :],
                        gu_sems.at[number],
                    )
                )
                down_copies.append(
                    pltpu.make_async_copy(
                        downs[rw].at[r],
                        down_s.at[:, pl.ds(pl.multiple_of(place * column, column), column)],
                        down_sems.at[number],
                    )
                )
    else:
        gate_copies.append(pltpu.make_async_copy(gates[0], gu_s, gu_sems.at[0]))
        down_copies.append(pltpu.make_async_copy(downs[0], down_s, down_sems.at[0]))
    for copy in gate_copies + down_copies:
        copy.start()
    for r in range(team):
        at = pl.ds(pl.multiple_of(jnp.bitwise_xor(t, r) * rows, rows), rows)
        mid = (
            streams[r][...].astype(F32)
            + (mine_ref[at, :].astype(F32) + other_ref[at, :].astype(F32))
        ).astype(BF)
        if r == 0:
            mid_s[...] = mid
        middle = mid.astype(F32)
        scaled = middle * lax.rsqrt(jnp.mean(middle * middle, axis=1, keepdims=True) + norm_eps)
        normed_s[at, :] = (scaled * gain_ref[...]).astype(BF)
    share = rows // tp
    mid_ref[...] = mid_s[pl.ds(pl.multiple_of(core * share, share), share), :]
    for copy in gate_copies:
        copy.wait()
    gate = jnp.dot(normed_s[...], gu_s[:, :units], preferred_element_type=F32)
    up = jnp.dot(normed_s[...], gu_s[:, units:], preferred_element_type=F32)
    hidden = (gate / (1.0 + jnp.exp(-gate)) * up).astype(BF)
    for copy in down_copies:
        copy.wait()
    width = min(512, depth)
    for n in range(0, depth, width):
        part = jnp.dot(hidden, down_s[:, pl.ds(n, width)], preferred_element_type=F32).astype(BF)
        for c in range(tp):
            for k in range(team):
                mixed_ref[c, k, :, pl.ds(n, width)] = part[
                    k * rows + c * share : k * rows + (c + 1) * share
                ]


def mixer(plan, place, gain, mine, other, streams, gates, downs):
    rows, depth = streams[0].shape
    total = plan.team * rows
    units = downs[0].shape[-2]
    share = rows // plan.tp
    pieces = plan.sp if plan.split else 1
    return pl.pallas_call(
        functools.partial(mixer_kernel, plan, len(gates), len(downs)),
        out_shape=(
            jax.ShapeDtypeStruct((share, depth), BF),
            jax.ShapeDtypeStruct((plan.tp, plan.team, share, depth), BF),
        ),
        in_specs=[SMEM] + [VMEM] * (3 + plan.team) + [ANY] * (len(gates) + len(downs)),
        out_specs=(VMEM, VMEM),
        scratch_shapes=[
            pltpu.VMEM((depth, 2 * units), BF),
            pltpu.VMEM((units, depth), BF),
            pltpu.VMEM((total, depth), BF),
            pltpu.VMEM((rows, depth), BF),
            pltpu.SemaphoreType.DMA((pieces,)),
            pltpu.SemaphoreType.DMA((pieces,)),
        ],
        cost_estimate=cost(6 * total * depth * units, 8 * total * depth),
        name="mixer",
    )(place, gain, mine, other, *streams, *gates, *downs)


def by_head(array, heads):
    rows = array.shape[0]
    return jnp.transpose(array.reshape(rows, heads, -1), (1, 0, 2))


def local(
    plan,
    stream,
    query_narrow,
    query_broad,
    key_narrow,
    key_broad,
    value_narrow,
    value_broad,
    key_offsets,
    out_narrow,
    out_broad,
    norm_gain,
    gate_weight,
    up_weight,
    down_weight,
):
    team, peers, tp = plan.team, plan.peers, plan.tp
    rows, depth = stream.shape
    heads = query_narrow.shape[1] // NARROW_SIZE
    i = lax.axis_index("sp").astype(jnp.int32)
    core = lax.axis_index("tp").astype(jnp.int32)
    t = plan.member(i)
    place = jnp.stack([i, core])

    narrow = functools.partial(by_head, heads=heads)
    body = jnp.concatenate(
        [
            narrow(key_broad),
            narrow(value_broad),
            narrow(key_narrow),
            narrow(value_narrow),
            narrow(query_broad),
            narrow(query_narrow),
            jnp.zeros((heads, rows, NARROW_SIZE), BF),
        ],
        axis=2,
    )
    high = lax.reduce_precision(key_offsets, 8, 7)
    middle = lax.reduce_precision(key_offsets - high, 8, 7)
    low = key_offsets - high - middle
    pieces = jnp.stack([high, middle, low]).astype(BF).reshape(3, rows, heads, 2)
    pieces = jnp.transpose(pieces, (2, 3, 0, 1))[:, ::-1].reshape(heads, 2, 3 * rows)
    tail = jnp.pad(pieces, ((0, 0), (0, EXTRA - 2), (0, ALL_LANES - 3 * rows)))
    packed = jnp.concatenate([body, tail], axis=1)
    packed = packed.reshape(team, heads // team, rows + EXTRA, ALL_LANES)

    units = gate_weight.shape[1] // team
    joined = jnp.concatenate(
        [
            jnp.transpose(gate_weight.reshape(-1, team, units), (1, 0, 2)),
            jnp.transpose(up_weight.reshape(-1, team, units), (1, 0, 2)),
        ],
        axis=2,
    )
    downs = down_weight.reshape(team, units, -1)

    if plan.split:
        own = [pick(packed, t)]
        own += [plan.team_swap(pick(packed, t ^ r), r) for r in range(1, team)]
        own = jnp.stack(own)
        keys = own[..., :KV_LANES]
        parts = [plan.peer_swap(keys, r) for r in range(1, peers)]
        streams = [stream] + [plan.team_swap(stream, r) for r in range(1, team)]
        gate_own = jnp.stack(
            [pick(joined, t)] + [plan.team_swap(pick(joined, t ^ r), r) for r in range(1, team)]
        )
        down_own = jnp.stack(
            [pick(downs, t)] + [plan.team_swap(pick(downs, t ^ r), r) for r in range(1, team)]
        )
        gates = [gate_own] + [plan.peer_swap(gate_own, r) for r in range(1, peers)]
        down_parts = [down_own] + [plan.peer_swap(down_own, r) for r in range(1, peers)]
    else:
        own = packed
        keys = own[0, :, :, :KV_LANES]
        parts = [lax.all_gather(keys, "sp", axis=0)]
        streams = [stream]
        gates = [lax.all_gather(joined[0], "sp", axis=0, tiled=True)]
        down_parts = [lax.all_gather(downs[0], "sp", axis=1, tiled=True)]

    mine = attention(plan, place, own, parts)
    attended = [mine] + [plan.team_swap(mine, r) for r in range(1, team)]
    partial = project(plan, place, attended, out_broad, out_narrow)
    if tp == 2:
        other = lax.ppermute(partial, "tp", [(0, 1), (1, 0)])
    else:
        summed = lax.psum(partial.astype(F32), "tp")
        partial, other = summed.astype(BF), jnp.zeros_like(partial)
    mid, mixed = mixer(
        plan, place, norm_gain.reshape(1, depth), partial, other, streams, gates, down_parts
    )
    sums = pick(mixed, core).astype(F32)
    if tp & (tp - 1) == 0:
        for c in range(1, tp):
            sent = lax.ppermute(pick(mixed, core ^ c), "tp", [(j, j ^ c) for j in range(tp)])
            sums = sums + sent.astype(F32)
    else:
        sums = lax.psum_scatter(mixed, "tp", scatter_dimension=0).astype(F32)
    sums = sums.astype(BF)
    result = mid.astype(F32) + pick(sums, t).astype(F32)
    for r in range(1, team):
        result = result + plan.team_swap(pick(sums, t ^ r), r).astype(F32)
    return result.astype(BF)


def solution(mesh):
    split = P("sp", "tp")
    placed = (P("sp", None),) + (split,) * 7 + (P("tp", None),) * 2 + (P(),)
    placed = placed + (split, split, P("tp", "sp"))
    sizes = dict(mesh.shape)

    def whole(*arrays):
        heads = arrays[1].shape[1] // NARROW_SIZE // sizes["tp"]
        hidden = arrays[11].shape[1] // sizes["tp"]
        plan = Plan(sizes["sp"], sizes["tp"], heads, hidden)
        return jax.shard_map(
            functools.partial(local, plan),
            mesh=mesh,
            in_specs=placed,
            out_specs=P(("sp", "tp"), None),
            check_vma=False,
        )(*arrays)

    return whole
```

```python
import functools

import jax
import jax.numpy as jnp
from jax import lax
from jax.experimental import pallas as pl
from jax.experimental.pallas import tpu as pltpu
from jax.sharding import PartitionSpec as P


NARROW_SIZE = 64
BROAD_SIZE = 128
LANES = 128
EXTRA = 8
KV_LANES = 2 * BROAD_SIZE + 2 * NARROW_SIZE
ALL_LANES = KV_LANES + BROAD_SIZE + 2 * NARROW_SIZE
norm_eps = 1e-06
NEG = -1e30
BF = jnp.bfloat16
F32 = jnp.float32
ANY = pl.BlockSpec(memory_space=pl.ANY)
VMEM = pl.BlockSpec(memory_space=pltpu.VMEM)
SMEM = pl.BlockSpec(memory_space=pltpu.SMEM)

TEAM_BITS = (2, 3)
PEER_BITS = (0, 1)


class Plan:
    def __init__(self, sp, tp, heads, hidden, depth):
        self.sp, self.tp = sp, tp
        self.split = sp == 16 and tp == 2 and heads % 4 == 0 and hidden % (4 * LANES) == 0
        self.split = self.split and depth == sp * LANES
        self.team_bits = TEAM_BITS if self.split else ()
        self.peer_bits = PEER_BITS if self.split else ()
        self.team = 4 if self.split else 1
        self.peers = sp // self.team

    def place(self, value, bits):
        out = 0
        for j, bit in enumerate(bits):
            out = out + (((value >> j) & 1) << bit)
        return out

    def index(self, t, w):
        if not self.split:
            return w
        return self.place(t, self.team_bits) + self.place(w, self.peer_bits)

    def member(self, i):
        if not self.split:
            return i * 0
        return sum(((i >> bit) & 1) << j for j, bit in enumerate(self.team_bits))

    def peer(self, i):
        if not self.split:
            return i
        return sum(((i >> bit) & 1) << j for j, bit in enumerate(self.peer_bits))

    def swap(self, array, offset):
        return lax.ppermute(array, "sp", [(i, i ^ offset) for i in range(self.sp)])

    def team_swap(self, array, r):
        return self.swap(array, self.place(r, self.team_bits))

    def peer_swap(self, array, r):
        return self.swap(array, self.place(r, self.peer_bits))


def pick(array, index):
    return lax.dynamic_index_in_dim(array, index, 0, keepdims=False)


def cost(flops, moved, transcendentals=0):
    return pl.CostEstimate(
        flops=int(flops), bytes_accessed=int(moved), transcendentals=int(transcendentals)
    )


def pack_kernel(plan, heads, me_ref, qn, qb, kn, kb, vn, vb, off_ref, *refs):
    outs, off_s = refs[: plan.team], refs[plan.team]
    rows = qb.shape[0]
    local_heads = heads // plan.team
    t = plan.member(me_ref[0])
    wide = jnp.concatenate(
        [off_ref[...], jnp.zeros((rows, LANES - off_ref.shape[1]), F32)], axis=1
    )
    off_s[...] = jnp.transpose(wide)

    def broad(ref, head):
        return ref[:, pl.ds(pl.multiple_of(head * BROAD_SIZE, BROAD_SIZE), BROAD_SIZE)]

    def narrow(ref, head):
        if heads == 1:
            return ref[...]
        both = ref[:, pl.ds(pl.multiple_of((head // 2) * LANES, LANES), LANES)].astype(F32)
        return jnp.where(head % 2 == 0, both[:, :NARROW_SIZE], both[:, NARROW_SIZE:]).astype(BF)

    for r in range(plan.team):
        for h in range(local_heads):
            head = jnp.bitwise_xor(t, r) * local_heads + h
            out = outs[r]
            out[h, pl.ds(0, rows), pl.ds(0, LANES)] = broad(kb, head)
            out[h, pl.ds(0, rows), pl.ds(LANES, LANES)] = broad(vb, head)
            out[h, pl.ds(0, rows), pl.ds(2 * LANES, LANES)] = jnp.concatenate(
                [narrow(kn, head), narrow(vn, head)], axis=1
            )
            out[h, pl.ds(0, rows), pl.ds(3 * LANES, LANES)] = broad(qb, head)
            out[h, pl.ds(0, rows), pl.ds(4 * LANES, LANES)] = jnp.concatenate(
                [narrow(qn, head), jnp.zeros((rows, NARROW_SIZE), BF)], axis=1
            )
            row = jnp.concatenate(
                [
                    off_s[pl.ds(2 * head + 1, 1), :],
                    off_s[pl.ds(2 * head, 1), :],
                    jnp.zeros((EXTRA - 2, rows), F32),
                ],
                axis=0,
            )
            high = row.astype(BF)
            rest = row - high.astype(F32)
            middle = rest.astype(BF)
            low = (rest - middle.astype(F32)).astype(BF)
            blank = jnp.zeros((EXTRA, ALL_LANES - 3 * rows), BF)
            out[h, pl.ds(rows, EXTRA), :] = jnp.concatenate([high, middle, low, blank], axis=1)


def pack(plan, me, heads, *arrays):
    rows = arrays[0].shape[0]
    shape = jax.ShapeDtypeStruct((heads // plan.team, rows + EXTRA, ALL_LANES), BF)
    return pl.pallas_call(
        functools.partial(pack_kernel, plan, heads),
        out_shape=[shape] * plan.team,
        in_specs=[SMEM] + [VMEM] * len(arrays),
        out_specs=[VMEM] * plan.team,
        scratch_shapes=[pltpu.VMEM((LANES, rows), F32)],
        cost_estimate=cost(1e6, 2e6),
        name="pack",
    )(me, *arrays)


def weights_kernel(plan, me_ref, gate, up, down, *outs):
    t = plan.member(me_ref[0])
    units = gate.shape[1] // plan.team
    band = gate.shape[0]
    for r in range(plan.team):
        at = pl.multiple_of(jnp.bitwise_xor(t, r) * units, LANES)
        outs[r][:, pl.ds(0, units)] = gate[:, pl.ds(at, units)]
        outs[r][:, pl.ds(units, units)] = up[:, pl.ds(at, units)]
        for j in range(units // band):
            start = pl.multiple_of(at + j * band, LANES)
            outs[r][:, pl.ds(2 * units + j * LANES, LANES)] = down[pl.ds(start, band), :]


def pack_weights(plan, me, gate, up, down):
    band, units = gate.shape[0], gate.shape[1] // plan.team
    shape = jax.ShapeDtypeStruct((band, 3 * units), BF)
    return pl.pallas_call(
        functools.partial(weights_kernel, plan),
        out_shape=[shape] * plan.team,
        in_specs=[SMEM] + [VMEM] * 3,
        out_specs=[VMEM] * plan.team,
        cost_estimate=cost(1e6, 4e6),
        name="pack_weights",
    )(me, gate, up, down)


def attention_kernel(plan, me_ref, own_ref, *refs):
    team, rows = plan.team, own_ref.shape[2] - EXTRA
    local_heads = own_ref.shape[1]
    part_count = plan.peers - 1 if plan.split else 1
    parts = refs[:part_count]
    out_ref, kv_s, q_s, acc_s, carry_s, kv_sems, q_sems = refs[part_count:]
    me = me_ref[0]
    t = plan.member(me)
    w = plan.peer(me)
    copies = []
    number = 0
    for h in range(local_heads):
        for r in range(team):
            copies.append(
                pltpu.make_async_copy(
                    own_ref.at[r, h, pl.ds(0, rows), pl.ds(KV_LANES, ALL_LANES - KV_LANES)],
                    q_s.at[h, jnp.bitwise_xor(t, r)],
                    q_sems.at[h * team + r],
                )
            )
        if plan.split:
            for rw in range(plan.peers):
                for r in range(team):
                    source = own_ref if rw == 0 else parts[rw - 1]
                    position = jnp.bitwise_xor(me, plan.index(r, rw))
                    copies.append(
                        pltpu.make_async_copy(
                            source.at[r, h, :, pl.ds(0, KV_LANES)],
                            kv_s.at[h, position],
                            kv_sems.at[number],
                        )
                    )
                    number += 1
        else:
            copies.append(
                pltpu.make_async_copy(parts[0].at[:, h], kv_s.at[h], kv_sems.at[number])
            )
            number += 1
    for copy in copies:
        copy.start()
    acc_s[...] = jnp.zeros_like(acc_s)
    carry_s[...] = jnp.zeros_like(carry_s)
    for copy in copies:
        copy.wait()

    pair = 2 if plan.sp % 2 == 0 else 1
    span = pair * rows
    tri = (
        lax.broadcasted_iota(jnp.int32, (span, span), 0)
        > lax.broadcasted_iota(jnp.int32, (span, span), 1)
    ).astype(F32).astype(BF)
    scales = (BROAD_SIZE ** (-0.5), NARROW_SIZE ** (-0.5))
    group = 2 if team % 2 == 0 else 1
    for first in reversed(range(0, team, group)):
        count = group * rows
        places = [plan.index(k, w) for k in range(first, first + group)]
        query_positions = jnp.concatenate(
            [p * rows + lax.broadcasted_iota(jnp.int32, (rows, span), 0) for p in places], axis=0
        )
        gap = lax.broadcasted_iota(jnp.int32, (count, span), 1) - query_positions
        steps = places[-1] // pair + 1

        def body(step, _, first=first, count=count, gap=gap, steps=steps):
            chunk = steps - 1 - step
            causal = gap < -chunk * span
            for h in range(local_heads):
                tails = [
                    kv_s[h, chunk * pair + b, pl.ds(rows, EXTRA), :].astype(F32)
                    for b in range(pair)
                ]
                tails = [a[:, :rows] + a[:, rows : 2 * rows] + a[:, 2 * rows : 3 * rows] for a in tails]
                offsets = jnp.concatenate(tails, axis=1)
                lanes = kv_s[h, pl.ds(chunk * pair, pair), pl.ds(0, rows), :]
                for g in range(2):
                    keys = lanes[:, :, 2 * LANES * g : 2 * LANES * g + LANES].reshape(span, LANES)
                    values = keys if g else lanes[:, :, LANES : 2 * LANES].reshape(span, LANES)
                    queries = q_s[h, first : first + group, :, g * LANES : (g + 1) * LANES]
                    queries = queries.reshape(count, LANES)
                    logits = lax.dot_general(
                        queries, keys, (((1,), (1,)), ((), ())), preferred_element_type=F32
                    )
                    logits = logits * scales[g] + offsets[g : g + 1]
                    logits = jnp.where(causal, logits, NEG)
                    lognot = jnp.minimum(-logits, 0.0) - jnp.log(1.0 + jnp.exp(-jnp.abs(logits)))
                    later = jnp.dot(lognot.astype(BF), tri, preferred_element_type=F32)
                    here = pl.ds(first * rows, count)
                    carry = carry_s[h, g, here, :]
                    wide = jnp.concatenate([carry] * (span // LANES), axis=1)
                    weights = jnp.exp(logits + lognot + (later + wide)).astype(BF)
                    acc_s[h, g, here, :] += jnp.dot(weights, values, preferred_element_type=F32)
                    carry_s[h, g, here, :] = carry + (later[:, :1] + lognot[:, :1])
            return 0

        lax.fori_loop(0, steps, body, 0)
    for h in range(local_heads):
        for g in range(2):
            out_ref[h, :, g * LANES : (g + 1) * LANES] = acc_s[h, g].astype(BF)


def attention(plan, me, own, parts):
    team, local_heads, tall, _ = own.shape
    rows = tall - EXTRA
    total = team * rows
    pieces = plan.sp if plan.split else 1
    work = local_heads * 2 * total * plan.sp * rows
    return pl.pallas_call(
        functools.partial(attention_kernel, plan),
        out_shape=jax.ShapeDtypeStruct((local_heads, total, 2 * LANES), BF),
        in_specs=[SMEM, ANY] + [ANY] * len(parts),
        out_specs=VMEM,
        scratch_shapes=[
            pltpu.VMEM((local_heads, plan.sp, tall, KV_LANES), BF),
            pltpu.VMEM((local_heads, team, rows, 2 * LANES), BF),
            pltpu.VMEM((local_heads, 2, total, LANES), F32),
            pltpu.VMEM((local_heads, 2, total, LANES), F32),
            pltpu.SemaphoreType.DMA((local_heads * pieces,)),
            pltpu.SemaphoreType.DMA((local_heads * team,)),
        ],
        cost_estimate=cost(work * 4 * LANES, 8 * own.size, 3 * work),
        name="attention",
    )(me, own, *parts)


def project_kernel(plan, me_ref, broad_ref, narrow_ref, *refs):
    team = plan.team
    attended, streams = refs[:team], refs[team : 2 * team]
    out_ref, a_s, w_s, stream_s = refs[2 * team :]
    rows, share = streams[0].shape
    for r in range(team):
        place = jnp.bitwise_xor(plan.member(me_ref[0]), r)
        stream_s[pl.ds(pl.multiple_of(place * rows, rows), rows), :] = streams[r][...]
    local_heads, _, _ = attended[0].shape
    t = plan.member(me_ref[0])
    depth = out_ref.shape[1]
    for r in range(team):
        for h in range(local_heads):
            at = (r * local_heads + h) * 2 * LANES
            head = jnp.bitwise_xor(t, r) * local_heads + h
            a_s[:, pl.ds(at, 2 * LANES)] = attended[r][h]
            w_s[pl.ds(at, LANES), :] = broad_ref[
                pl.ds(pl.multiple_of(head * BROAD_SIZE, BROAD_SIZE), BROAD_SIZE), :
            ]
            w_s[pl.ds(at + LANES, NARROW_SIZE), :] = jnp.zeros((NARROW_SIZE, depth), BF)
            w_s[pl.ds(at + LANES + NARROW_SIZE, NARROW_SIZE), :] = narrow_ref[
                pl.ds(pl.multiple_of(head * NARROW_SIZE, NARROW_SIZE), NARROW_SIZE), :
            ]
    width = min(512, share)
    for n in range(0, depth, width):
        mine = (me_ref[1] == n // share).astype(F32)
        part = jnp.dot(a_s[...], w_s[:, pl.ds(n, width)], preferred_element_type=F32)
        part = part + mine * stream_s[:, pl.ds(n % share, width)].astype(F32)
        out_ref[:, pl.ds(n, width)] = part.astype(BF)


def project(plan, me, attended, streams, out_broad, out_narrow):
    local_heads, total, _ = attended[0].shape
    depth = out_broad.shape[1]
    inner = plan.team * local_heads * 2 * LANES
    return pl.pallas_call(
        functools.partial(project_kernel, plan),
        out_shape=jax.ShapeDtypeStruct((total, depth), BF),
        in_specs=[SMEM] + [VMEM] * (2 + 2 * len(attended)),
        out_specs=VMEM,
        scratch_shapes=[
            pltpu.VMEM((total, inner), BF),
            pltpu.VMEM((inner, depth), BF),
            pltpu.VMEM((total, streams[0].shape[1]), BF),
        ],
        cost_estimate=cost(2 * total * inner * depth, 2 * total * depth),
        name="project",
    )(me, out_broad, out_narrow, *attended, *streams)


def mixer_kernel(plan, weight_parts, me_ref, gain_ref, mine_ref, other_ref, *refs):
    team, tp = plan.team, plan.tp
    weights, refs = refs[:weight_parts], refs[weight_parts:]
    mid_ref, mixed_ref, gu_s, down_s, normed_s, mid_s, gu_sems, down_sems = refs
    me, core = me_ref[0], me_ref[1]
    t = plan.member(me)
    total, depth = mine_ref.shape
    rows = total // team
    band = depth // plan.sp
    units = down_s.shape[0]
    gate_copies, down_copies = [], []
    if plan.split:
        for part, (half, rw) in enumerate(WEIGHT_PARTS):
            for s in range(2):
                place = pl.multiple_of(
                    jnp.bitwise_xor(me, plan.index(2 * half + s, rw)) * band, band
                )
                number = 2 * part + s
                gate_copies.append(
                    pltpu.make_async_copy(
                        weights[part].at[s, :, pl.ds(0, 2 * units)],
                        gu_s.at[pl.ds(place, band), :],
                        gu_sems.at[number],
                    )
                )
                for j in range(units // band):
                    down_copies.append(
                        pltpu.make_async_copy(
                            weights[part].at[s, :, pl.ds(2 * units + j * band, band)],
                            down_s.at[pl.ds(j * band, band), pl.ds(place, band)],
                            down_sems.at[number * (units // band) + j],
                        )
                    )
    else:
        gate_copies.append(
            pltpu.make_async_copy(weights[0], gu_s.at[:, pl.ds(0, units)], gu_sems.at[0])
        )
        gate_copies.append(
            pltpu.make_async_copy(weights[1], gu_s.at[:, pl.ds(units, units)], gu_sems.at[1])
        )
        down_copies.append(pltpu.make_async_copy(weights[2], down_s, down_sems.at[0]))
    for copy in gate_copies + down_copies:
        copy.start()
    for k in range(team):
        at = pl.ds(k * rows, rows)
        middle = (mine_ref[at, :].astype(F32) + other_ref[at, :].astype(F32)).astype(BF)
        mid_s[at, :] = middle
        middle = middle.astype(F32)
        scaled = middle * lax.rsqrt(jnp.mean(middle * middle, axis=1, keepdims=True) + norm_eps)
        normed_s[at, :] = (scaled * gain_ref[...]).astype(BF)
    share = rows // tp
    mid_ref[...] = mid_s[pl.ds(pl.multiple_of(t * rows + core * share, share), share), :]
    for copy in gate_copies:
        copy.wait()
    gate = jnp.dot(normed_s[...], gu_s[:, :units], preferred_element_type=F32)
    up = jnp.dot(normed_s[...], gu_s[:, units:], preferred_element_type=F32)
    hidden = (gate / (1.0 + jnp.exp(-gate)) * up).astype(BF)
    for copy in down_copies:
        copy.wait()
    width = min(512, depth)
    for n in range(0, depth, width):
        part = jnp.dot(hidden, down_s[:, pl.ds(n, width)], preferred_element_type=F32).astype(BF)
        for c in range(tp):
            for k in range(team):
                mixed_ref[c, k, :, pl.ds(n, width)] = part[
                    k * rows + c * share : k * rows + (c + 1) * share
                ]


WEIGHT_PARTS = ((0, 0), (1, 0), (0, 1), (1, 2), (0, 2), (1, 1), (0, 3), (1, 3))


def mixer(plan, place, gain, mine, other, units, weights):
    total, depth = mine.shape
    share = total // plan.team // plan.tp
    return pl.pallas_call(
        functools.partial(mixer_kernel, plan, len(weights)),
        out_shape=(
            jax.ShapeDtypeStruct((share, depth), BF),
            jax.ShapeDtypeStruct((plan.tp, plan.team, share, depth), BF),
        ),
        in_specs=[SMEM] + [VMEM] * 3 + [ANY] * len(weights),
        out_specs=(VMEM, VMEM),
        scratch_shapes=[
            pltpu.VMEM((depth, 2 * units), BF),
            pltpu.VMEM((units, depth), BF),
            pltpu.VMEM((total, depth), BF),
            pltpu.VMEM((total, depth), BF),
            pltpu.SemaphoreType.DMA((2 * len(weights),)),
            pltpu.SemaphoreType.DMA((2 * len(weights) * max(1, units // LANES),)),
        ],
        cost_estimate=cost(6 * total * depth * units, 8 * total * depth),
        name="mixer",
    )(place, gain, mine, other, *weights)


def local(
    plan,
    stream,
    query_narrow,
    query_broad,
    key_narrow,
    key_broad,
    value_narrow,
    value_broad,
    key_offsets,
    out_narrow,
    out_broad,
    norm_gain,
    gate_weight,
    up_weight,
    down_weight,
):
    return layer(
        plan,
        stream,
        query_narrow,
        query_broad,
        key_narrow,
        key_broad,
        value_narrow,
        value_broad,
        key_offsets,
        out_narrow,
        out_broad,
        norm_gain,
        gate_weight,
        up_weight,
        down_weight,
    )


def layer(
    plan,
    stream,
    query_narrow,
    query_broad,
    key_narrow,
    key_broad,
    value_narrow,
    value_broad,
    key_offsets,
    out_narrow,
    out_broad,
    norm_gain,
    gate_weight,
    up_weight,
    down_weight,
):
    team, peers, tp = plan.team, plan.peers, plan.tp
    _, depth = stream.shape
    heads = query_narrow.shape[1] // NARROW_SIZE
    i = lax.axis_index("sp").astype(jnp.int32)
    core = lax.axis_index("tp").astype(jnp.int32)
    t = plan.member(i)
    place = jnp.stack([i, core])

    width = depth // tp
    stream = lax.dynamic_slice_in_dim(stream, core * width, width, 1)
    units = gate_weight.shape[1] // team
    packed = pack(
        plan,
        place,
        heads,
        query_narrow,
        query_broad,
        key_narrow,
        key_broad,
        value_narrow,
        value_broad,
        key_offsets,
    )
    if plan.split:
        own = [packed[0]] + [plan.team_swap(packed[r], r) for r in range(1, team)]
        own = jnp.stack(own)
        keys = own[..., :KV_LANES]
        parts = [plan.peer_swap(keys, r) for r in range(1, peers)]
        slots = pack_weights(plan, place, gate_weight, up_weight, down_weight)
        slots = [slots[0]] + [plan.team_swap(slots[r], r) for r in range(1, team)]
        streams = [stream] + [plan.team_swap(stream, r) for r in range(1, team)]
        left, right = jnp.stack(slots[:2]), jnp.stack(slots[2:])
        left1 = plan.peer_swap(left, 1)
        right2 = plan.peer_swap(right, 2)
        left2 = plan.peer_swap(left, 2)
        right1 = plan.peer_swap(right, 1)
        left3 = plan.peer_swap(left1, 2)
        right3 = plan.peer_swap(right2, 1)
        weights = [left, right, left1, right2, left2, right1, left3, right3]
    else:
        own = jnp.stack(packed)
        keys = own[0, :, :, :KV_LANES]
        parts = [lax.all_gather(keys, "sp", axis=0)]
        streams = [stream]
        weights = [
            lax.all_gather(gate_weight, "sp", axis=0, tiled=True),
            lax.all_gather(up_weight, "sp", axis=0, tiled=True),
            lax.all_gather(down_weight, "sp", axis=1, tiled=True),
        ]

    mine = attention(plan, place, own, parts)
    attended = [mine]
    attended += [plan.team_swap(mine, r) for r in range(1, team)]
    partial = project(plan, place, attended, streams, out_broad, out_narrow)
    if tp == 2:
        other = lax.ppermute(partial, "tp", [(0, 1), (1, 0)])
    else:
        summed = lax.psum(partial.astype(F32), "tp")
        partial, other = summed.astype(BF), jnp.zeros_like(partial)
    mid, mixed = mixer(plan, place, norm_gain.reshape(1, depth), partial, other, units, weights)
    sums = pick(mixed, core).astype(F32)
    if tp & (tp - 1) == 0:
        for c in range(1, tp):
            sent = lax.ppermute(pick(mixed, core ^ c), "tp", [(j, j ^ c) for j in range(tp)])
            sums = sums + sent.astype(F32)
    else:
        sums = lax.psum_scatter(mixed, "tp", scatter_dimension=0).astype(F32)
    sums = sums.astype(BF)
    result = mid.astype(F32) + pick(sums, t).astype(F32)
    for r in range(1, team):
        result = result + plan.team_swap(pick(sums, t ^ r), r).astype(F32)
    return result.astype(BF)


def solution(mesh):
    split = P("sp", "tp")
    placed = (P("sp", None),) + (split,) * 7 + (P("tp", None),) * 2 + (P(),)
    placed = placed + (split, split, P("tp", "sp"))
    sizes = dict(mesh.shape)

    def whole(*arrays):
        heads = arrays[1].shape[1] // NARROW_SIZE // sizes["tp"]
        hidden = arrays[11].shape[1] // sizes["tp"]
        plan = Plan(sizes["sp"], sizes["tp"], heads, hidden, arrays[0].shape[1])
        step = jax.shard_map(
            functools.partial(local, plan),
            mesh=mesh,
            in_specs=placed,
            out_specs=P(("sp", "tp"), None),
            check_vma=False,
        )
        return step(*arrays)

    return whole
```
